512 devices in a mesh: kv: 128 (over z, y, core), tp: 4 (over x).
Axes of the slice: x: 4, y: 8, z: 8, core: 2. Of those that a mesh axis runs over, the one named last changes fastest.
Arguments:
- piece_tokens: bfloat16 [512, 2048], P('kv'), may hold values from -6 to 6
- decode_tokens: bfloat16 [128, 2048], P('kv'), may hold values from -6 to 6
- prompt_fill: int32 [1], replicated, may hold values from 16384 to 32256
- decode_fill: int32 [128], P('kv'), may hold values from 1 to 767, 49152 in all
- prompt_cache: bfloat16 [32768, 544], P('kv'), may hold values from -600 to 600
- decode_cache: bfloat16 [128, 768, 544], P('kv'), may hold values from -600 to 600
- input_gain: float32 [2048], replicated, may hold values from 0.1 to 1.9
- query_gain: float32 [768], replicated, may hold values from 0.1 to 1.9
- latent_gain: float32 [512], replicated, may hold values from 0.1 to 1.9
- query_down: bfloat16 [2048, 768], P(None, 'tp'), may hold values from -0.125 to 0.125
- latent_down: bfloat16 [2048, 512], P(None, 'tp'), may hold values from -0.125 to 0.125
- rope_down: bfloat16 [2048, 32], replicated, may hold values from -0.125 to 0.125
- query_up: bfloat16 [768, 1024], P(None, 'tp'), may hold values from -0.21875 to 0.21875
- qrope_up: bfloat16 [768, 512], P(None, 'tp'), may hold values from -0.21875 to 0.21875
- key_up: bfloat16 [16, 64, 512], P('tp'), may hold values from -0.25 to 0.25
- value_up: bfloat16 [16, 512, 64], P('tp'), may hold values from -4 to 4
- out_proj: bfloat16 [1024, 2048], P('tp'), may hold values from -4 to 4
Outputs:
- piece_out: bfloat16 [512, 2048], P('kv')
- decode_out: bfloat16 [128, 2048], P('kv')
- piece_rows: bfloat16 [512, 544], P('kv')
- decode_rows: bfloat16 [128, 544], P('kv')
The draws below stay inside these ranges and needn't reach their ends.
Inputs may be any that keep to these rules, and one draw needn't show every extreme that they name: `prompt_fill`: the piece takes the 512 positions that follow the cache's filled positions. `decode_fill`: a decoding sequence's new token takes the position that follows its filled ones.
All inputs are finite; a program needn't handle non-finite values. No bound on the sum of `decode_fill` on one device may be relied on, other than what follows from the above.
Results may differ from the reference program's by a relative error of at most 0.035.
Values may be sent and summed in bfloat16 or wider, within the bound.
A program may use at most 64 MiB of HBM per device.

```python
import math
import jax
import jax.numpy as jnp
import numpy as np
from jax import lax

D = 2048
H = 16
QL = 768
KL = 512
NOPE = 64
ROPE = 32
VD = 64
CACHE_DEV = 256
DEC_LEN = 768
PIECE = 512
CACHE = 32768
DEC = 128
N_KV = 128
N_TP = 4


def draw_prompt_cache(key, part):
    values = jnp.clip(jax.random.normal(key, (CACHE, KL + ROPE), jnp.float32), -5.0, 5.0)
    return values.astype(jnp.bfloat16)


def draw_decode_cache(key, part):
    values = jnp.clip(jax.random.normal(key, (DEC, DEC_LEN, KL + ROPE), jnp.float32), -5.0, 5.0)
    return values.astype(jnp.bfloat16)


def block_levels(key, dims, pieces, least, largest):
    def one(position, shards_of):
        draws = jax.random.uniform(jax.random.fold_in(jax.random.fold_in(key, 6), position), (shards_of,), jnp.float32, least / len(pieces), largest / len(pieces))
        return jnp.repeat(jnp.exp(draws), dims[position] // shards_of).reshape((-1,) + (1,) * (len(dims) - position - 1))

    gain = one(*pieces[0])
    for cut in pieces[1:]:
        gain = gain * one(*cut)
    return gain


def profile(amount, total, most, slope):
    weights = [(1 << 20) // math.isqrt(grade ** slope) + 1 for grade in range(2, amount + 1)]
    rest, holding = total - most - (amount - 1), [1] * (amount - 1)
    while rest > 0:
        candidates = [i for i in range(amount - 1) if holding[i] < most]
        whole, left = sum([weights[i] for i in candidates]), rest
        for i in candidates:
            extra = min(most - holding[i], max(1, left * weights[i] // whole), rest)
            holding[i] = holding[i] + extra
            rest = rest - extra
    return np.array([most] + holding)


def uneven(rng, amount, total, most, skew):
    if amount == 2:
        one = jax.random.randint(rng, (), max(1, total - most), min(most, total - 1) + 1)
        return jnp.stack([one, total - one])
    tallies = jnp.asarray(profile(amount, total, most, skew), jnp.int32)
    couples = (amount - 1) // 2
    donor, receiver = tallies[1:1 + 2 * couples:2], tallies[2:2 + 2 * couples:2]
    margin = jnp.minimum(donor - 1, most - receiver)
    moved = jax.random.randint(jax.random.fold_in(rng, 1), (couples,), 0, 1 << 20) % (margin + 1)
    tallies = tallies.at[1:1 + 2 * couples:2].set(donor - moved).at[2:2 + 2 * couples:2].set(receiver + moved)
    return tallies[jax.random.permutation(jax.random.fold_in(rng, 2), amount)]


def gaussian(stream_key, dims, scale, most, split=(), held_as=jnp.bfloat16):
    result = scale * jax.random.normal(stream_key, dims, jnp.float32)
    if split:
        result = result * block_levels(stream_key, dims, split, -0.22, 0.18)
    return jnp.clip(result, -most, most).astype(held_as)


def setup_inputs(seed: int = 0) -> dict:
    key_of = jax.random.split(jax.random.key(seed), 18)
    return {
        "piece_tokens": gaussian(key_of[0], (PIECE, D), 1.0, 6.0, ((0, 128),)),
        "decode_tokens": gaussian(key_of[1], (DEC, D), 1.0, 6.0, ((0, 128),)),
        "prompt_fill": jax.random.randint(key_of[2], (1,), CACHE // 2, CACHE - PIECE + 1).astype(jnp.int32),
        "decode_fill": uneven(key_of[3], DEC, DEC * DEC_LEN // 2, DEC_LEN - 1, 2).astype(jnp.int32),
        "prompt_cache": draw_prompt_cache(jax.random.fold_in(key_of[17], 71), 0),
        "decode_cache": draw_decode_cache(jax.random.fold_in(key_of[17], 71), 0),
        "input_gain": jnp.clip(1.0 + 0.18 * jax.random.normal(key_of[6], (D,), jnp.float32), 0.1, 1.9),
        "query_gain": jnp.clip(1.0 + 0.18 * jax.random.normal(key_of[7], (QL,), jnp.float32), 0.1, 1.9),
        "latent_gain": jnp.clip(1.0 + 0.18 * jax.random.normal(key_of[8], (KL,), jnp.float32), 0.1, 1.9),
        "query_down": gaussian(key_of[9], (D, QL), D ** -0.5, 0.125, ((1, 4),)),
        "latent_down": gaussian(key_of[10], (D, KL), D ** -0.5, 0.125, ((1, 4),)),
        "rope_down": gaussian(key_of[11], (D, ROPE), D ** -0.5, 0.125),
        "query_up": gaussian(key_of[12], (QL, H * NOPE), QL ** -0.5, 0.21875, ((1, 4),)),
        "qrope_up": gaussian(key_of[13], (QL, H * ROPE), QL ** -0.5, 0.21875, ((1, 4),)),
        "key_up": gaussian(key_of[14], (H, NOPE, KL), KL ** -0.5, 0.25, ((0, 4),)),
        "value_up": gaussian(key_of[15], (H, KL, VD), 0.25, 4.0, ((0, 4),)),
        "out_proj": gaussian(key_of[16], (H * VD, D), 0.25, 4.0, ((0, 4),)),
    }


NEG_FILL = -1e+30
RMS_EPS = 1e-06
THETA = 10000.0

def rms_scale(values, gain_row):
    widened = values.astype(jnp.float32)
    scaled = widened * lax.rsqrt(lax.optimization_barrier(jnp.mean(widened * widened, axis=-1, keepdims=True)) + RMS_EPS) * gain_row.astype(jnp.float32)
    return scaled.astype(jnp.bfloat16)

def rotate(values, places):
    half_width = values.shape[-1] // 2
    inverse = THETA ** (-jnp.arange(half_width, dtype=jnp.float32) / half_width)
    angles = places.astype(jnp.float32)[..., None] * inverse
    first_half = values[..., :half_width].astype(jnp.float32)
    second_half = values[..., half_width:].astype(jnp.float32)
    cosine = jnp.cos(angles)
    sine_part = jnp.sin(angles)
    return jnp.concatenate([first_half * cosine - second_half * sine_part, first_half * sine_part + second_half * cosine], axis=-1).astype(jnp.bfloat16)

def project(tokens, places, input_gain, query_gain, latent_gain, query_down, latent_down, rope_down):
    normed = rms_scale(tokens, input_gain)
    query_comp = jnp.dot(normed, query_down, preferred_element_type=jnp.float32).astype(jnp.bfloat16)
    latent_comp = jnp.dot(normed, latent_down, preferred_element_type=jnp.float32).astype(jnp.bfloat16)
    rope_raw = jnp.dot(normed, rope_down, preferred_element_type=jnp.float32).astype(jnp.bfloat16)
    new_rows = jnp.concatenate([rms_scale(latent_comp, latent_gain), rotate(rope_raw, places)], axis=-1)
    return (rms_scale(query_comp, query_gain), new_rows)

def make_queries(query_lat, places, query_up, qrope_up, key_up):
    row_count = query_lat.shape[0]
    head_count = key_up.shape[0]
    nope_part = jnp.dot(query_lat, query_up, preferred_element_type=jnp.float32).astype(jnp.bfloat16).reshape(row_count, head_count, -1)
    rope_raw = jnp.dot(query_lat, qrope_up, preferred_element_type=jnp.float32).astype(jnp.bfloat16).reshape(row_count, head_count, -1)
    turned = rotate(rope_raw, places[:, None])
    absorbed = jnp.einsum('nhc,hcl->nhl', nope_part.astype(jnp.float32), key_up.astype(jnp.float32)).astype(jnp.bfloat16)
    return (absorbed, turned)

def block_attend(absorbed, turned, key_rows, key_places, query_places, value_up):
    latent_width = value_up.shape[1]
    score_scale = (NOPE + ROPE) ** (-0.5)
    latent_keys = key_rows[:, :latent_width].astype(jnp.float32)
    scores = (jnp.einsum('nhl,sl->nhs', absorbed.astype(jnp.float32), latent_keys) + jnp.einsum('nhr,sr->nhs', turned.astype(jnp.float32), key_rows[:, latent_width:].astype(jnp.float32))) * score_scale
    allowed = key_places[None, None, :] <= query_places[:, None, None]
    scores = jnp.where(allowed, scores, NEG_FILL)
    local_peak = lax.optimization_barrier(jnp.max(scores, axis=-1))
    exp_scores = jnp.where(allowed, jnp.exp(scores - local_peak[..., None]), 0.0)
    weight_sum = lax.optimization_barrier(jnp.sum(exp_scores, axis=-1))
    weights = lax.optimization_barrier(exp_scores.astype(jnp.bfloat16)).astype(jnp.float32)
    mixed_rows = jnp.einsum('nhs,sl->nhl', weights, latent_keys)
    partial_sum = jnp.einsum('nhl,hlv->nhv', mixed_rows, value_up.astype(jnp.float32), precision=lax.Precision.HIGHEST)
    return (partial_sum, weight_sum, local_peak)

def insert_row(cache_rows, new_row, fill_one):
    return lax.dynamic_update_slice(cache_rows, new_row[None], (fill_one.astype(jnp.int32), jnp.zeros((), jnp.int32)))

def project_out(values, out_proj):
    row_count = values.shape[0]
    grouped = values.reshape(row_count, N_TP, -1).astype(jnp.float32)
    weight_groups = out_proj.reshape(N_TP, -1, out_proj.shape[1]).astype(jnp.float32)
    group_out = jnp.einsum('ngk,gkd->ngd', grouped, weight_groups).astype(jnp.bfloat16)
    group_out = lax.optimization_barrier(group_out).astype(jnp.float32)
    return lax.optimization_barrier(jnp.sum(group_out, axis=1)).astype(jnp.bfloat16)

def reference(piece_tokens, decode_tokens, prompt_fill, decode_fill, prompt_cache, decode_cache, input_gain, query_gain, latent_gain, query_down, latent_down, rope_down, query_up, qrope_up, key_up, value_up, out_proj):
    fill_start = prompt_fill[0].astype(jnp.int32)
    piece_places = fill_start + jnp.arange(PIECE, dtype=jnp.int32)
    decode_places = decode_fill.astype(jnp.int32)
    piece_lat, piece_rows = project(piece_tokens, piece_places, input_gain, query_gain, latent_gain, query_down, latent_down, rope_down)
    decode_lat, decode_rows = project(decode_tokens, decode_places, input_gain, query_gain, latent_gain, query_down, latent_down, rope_down)
    piece_absorbed, piece_turned = make_queries(piece_lat, piece_places, query_up, qrope_up, key_up)
    decode_absorbed, decode_turned = make_queries(decode_lat, decode_places, query_up, qrope_up, key_up)
    full_cache = lax.dynamic_update_slice(prompt_cache, piece_rows, (fill_start, jnp.zeros((), jnp.int32)))
    head_count = key_up.shape[0]
    value_width = value_up.shape[2]

    def step(carry, block_index):
        peak_run, numer_run, denom_run = carry
        key_rows = lax.dynamic_slice_in_dim(full_cache, block_index * CACHE_DEV, CACHE_DEV, 0)
        key_places = block_index * CACHE_DEV + jnp.arange(CACHE_DEV, dtype=jnp.int32)
        partial_sum, weight_sum, local_peak = block_attend(piece_absorbed, piece_turned, key_rows, key_places, piece_places, value_up)
        new_peak = jnp.maximum(peak_run, local_peak)
        old_factor = jnp.exp(peak_run - new_peak)
        new_factor = jnp.exp(local_peak - new_peak)
        numer_run = numer_run * old_factor[..., None] + partial_sum * new_factor[..., None]
        denom_run = denom_run * old_factor + weight_sum * new_factor
        return ((new_peak, numer_run, denom_run), None)
    start_carry = (jnp.full((PIECE, head_count), NEG_FILL, jnp.float32), jnp.zeros((PIECE, head_count, value_width), jnp.float32), jnp.zeros((PIECE, head_count), jnp.float32))
    final_carry, unused = lax.scan(step, start_carry, jnp.arange(N_KV, dtype=jnp.int32))
    piece_value = (final_carry[1] / final_carry[2][..., None]).astype(jnp.bfloat16)
    decode_keys = jax.vmap(insert_row)(decode_cache, decode_rows, decode_places)

    def attend_one(absorbed_one, turned_one, keys_one, fill_one):
        key_places = jnp.arange(keys_one.shape[0], dtype=jnp.int32)
        return block_attend(absorbed_one[None], turned_one[None], keys_one, key_places, fill_one[None], value_up)
    decode_part, decode_total, decode_peak = jax.vmap(attend_one)(decode_absorbed, decode_turned, decode_keys, decode_places)
    decode_value = (decode_part[:, 0] / decode_total[:, 0, :, None]).astype(jnp.bfloat16)
    piece_out = project_out(piece_value.reshape(PIECE, -1), out_proj)
    decode_out = project_out(decode_value.reshape(decode_value.shape[0], -1), out_proj)
    return (piece_out, decode_out, piece_rows, decode_rows)
```

```python
import functools

import jax
import jax.numpy as jnp
from jax import lax
from jax.experimental import pallas as pl
from jax.experimental.pallas import tpu as pltpu
from jax.sharding import PartitionSpec as P

MESH = pl.DeviceIdType.MESH
NEG = -1e30
EPS = 1e-06
LOG2E = 1.4426950408889634
SCALE = (64 + 32) ** (-0.5) * LOG2E
INVERSE = tuple(float(10000.0 ** (-i / 16)) for i in range(16))
BF = jnp.bfloat16
F32 = jnp.float32


def dot(a, b):
    return jnp.dot(a, b, preferred_element_type=F32)


def dot_t(a, b):
    return lax.dot_general(a, b, (((1,), (1,)), ((), ())), preferred_element_type=F32)


def angles(places):
    lane = lax.broadcasted_iota(jnp.int32, (8, 128), 1)
    step = lax.rem(lane, 16)
    inverse = jnp.full((8, 128), INVERSE[0], F32)
    for i in range(1, 16):
        inverse = jnp.where(step == i, INVERSE[i], inverse)
    turn = places.astype(F32) * inverse
    sine = jnp.sin(turn)
    return jnp.cos(turn), jnp.where(lax.rem(lane, 32) < 16, -sine, sine)


def rotate(values, cosine, sine):
    lane = lax.broadcasted_iota(jnp.int32, (8, 128), 1)
    other = jnp.where(
        lax.rem(lane, 32) < 16, pltpu.roll(values, 112, 1), pltpu.roll(values, 16, 1)
    )
    return values * cosine + other * sine


def kernel(
    nz, ny, ntp,
    fill_any, dfill_any, piece_any, dec_any, ingain_any, qgain_any, lgain_any,
    qd_any, ld_any, rd_any, qu_any, qr_any, ku_any, vu_any, op_any, pc_any, dc_any,
    piece_out, dec_out, piece_rows, dec_rows,
    fill_v, dfill_v, piece_v, dec_v, ingain_v, qgain_v, lgain_v,
    qd, ld, rd, qu, qr, ku, vu, op, pc, dc,
    partner, xs, cbuf, nb, qs, kbuf, vbuf, qbuf, rsend, rbuf, mid, vs, obuf, dbuf,
    chip_in, line_in, all_in,
    load_sem, c_send, c_recv, p_send, p_recv, n_send, n_recv,
    q_send, q_recv, r_send, r_recv, o_send, o_recv, d_send, d_recv,
):
    kv, tp = lax.axis_index("kv"), lax.axis_index("tp")
    chip, core = lax.div(kv, 2), lax.rem(kv, 2)
    z, y = lax.div(chip, ny), lax.rem(chip, ny)
    peers = nz * ny - 1
    other_kv = chip * 2 + (1 - core)

    pairs = (
        (piece_any, piece_v), (dec_any, dec_v), (ingain_any, ingain_v), (qd_any, qd),
        (ld_any, ld), (pc_any, pc), (ku_any, ku), (vu_any, vu), (rd_any, rd),
        (fill_any, fill_v), (dfill_any, dfill_v), (qgain_any, qgain_v), (lgain_any, lgain_v),
        (qu_any, qu), (qr_any, qr), (dc_any, dc), (op_any, op),
    )
    loads = [pltpu.make_async_copy(a, v, load_sem.at[i]) for i, (a, v) in enumerate(pairs)]
    for load in loads:
        load.start()

    barrier = pltpu.get_barrier_semaphore()

    z_part = [lax.rem(z + d, nz) * (2 * ny) + core for d in range(nz)]
    y_part = [lax.rem(y + d, ny) * 2 for d in range(ny)]

    def targets():
        def far(step):
            dz, dy = step
            return -(min(dz, nz - dz) + min(dy, ny - dy))

        steps = [(dz, dy) for dz in range(nz) for dy in range(ny)][1:]
        for dz, dy in sorted(steps, key=far):
            yield z_part[dz] + y_part[dy], dz * ny + dy, (-dz % nz) * ny + -dy % ny

    def tell(sem, kv_t, tp_t):
        pl.semaphore_signal(sem, inc=1, device_id=(kv_t, tp_t), device_id_type=MESH)

    @pl.when(core == 0)
    def _():
        for j in range(1, ntp):
            tell(barrier, kv, lax.rem(tp + j, ntp))
        pl.semaphore_wait(barrier, ntp)
        tell(chip_in, other_kv, tp)
        for j in range(1, ntp):
            tell(line_in, kv, lax.rem(tp + j, ntp))

    @pl.when(core == 1)
    def _():
        tell(barrier, other_kv, tp)
        pl.semaphore_wait(chip_in, 1)
        for kv_t, unused, unused_too in targets():
            tell(barrier, kv_t, tp)

    xs[...] = jnp.zeros(xs.shape, F32)
    for load in loads[:5]:
        load.wait()
    xs[0:4] = piece_v[...].astype(F32)
    xs[4:5] = dec_v[...].astype(F32)
    x = xs[...]
    mean = jnp.mean(x * x, axis=-1, keepdims=True)
    normed = (x * lax.rsqrt(mean + EPS) * ingain_v[...]).astype(BF)
    cbuf[tp, :, 0:128] = dot(normed, ld[...]).astype(BF)
    cbuf[tp, :, 128:320] = dot_t(normed, qd[...]).astype(BF)

    zeros = jnp.zeros((32, kbuf.shape[2]), BF)
    row = lax.broadcasted_iota(jnp.int32, (64, vbuf.shape[2]), 0)
    ones = jnp.where((row == 0) | (row == 4), 1.0, 0.0).astype(BF)
    for h in range(4):
        kbuf[h, 96:128] = zeros
        vbuf[h, 64:128] = ones
    nb[0:16] = jnp.zeros((16, 640), BF)
    nb[32:128] = jnp.zeros((96, 640), BF)
    for load in loads[5:9]:
        load.wait()

    def expand(rows, at):
        latent = rows[0:512]
        keys = dot(ku[...], latent).astype(BF)
        vals = dot(vu[...], latent).astype(BF)
        turned_keys = rows[512:544]
        for h in range(4):
            kbuf[h, 0:64, at : at + 256] = keys[64 * h : 64 * h + 64]
            kbuf[h, 64:96, at : at + 256] = turned_keys
            vbuf[h, 0:64, at : at + 256] = vals[64 * h : 64 * h + 64]

    expand(pc, 0)
    rope_raw = dot_t(normed, rd[...]).astype(BF).astype(F32)
    for load in loads[9:]:
        load.wait()
    fill, dfill = fill_v[...], dfill_v[...]
    token_row = lax.broadcasted_iota(jnp.int32, (8, 128), 0)
    places = jnp.where(token_row < 4, fill + kv * 4 + token_row, dfill)
    cosine, sine = angles(places)
    rope_row = rotate(
        jnp.concatenate([rope_raw, jnp.zeros((8, 96), F32)], axis=1), cosine, sine
    ).astype(BF)

    @pl.when(core == 0)
    def _():
        pl.semaphore_wait(line_in, ntp - 1)
        tell(chip_in, other_kv, tp)

    @pl.when(core == 1)
    def _():
        pl.semaphore_wait(chip_in, 1)

    def to_tp(src, dst, send, recv):
        copies = []
        for j in range(1, ntp):
            copies.append(
                pltpu.make_async_remote_copy(
                    src_ref=src, dst_ref=dst, send_sem=send, recv_sem=recv,
                    device_id=(kv, lax.rem(tp + j, ntp)), device_id_type=MESH,
                )
            )
            copies[-1].start()

    def to_partner(src, dst, send, recv):
        return pltpu.make_async_remote_copy(
            src_ref=src, dst_ref=dst, send_sem=send, recv_sem=recv,
            device_id=(other_kv, tp), device_id_type=MESH,
        )

    def many(ref, send, recv):
        return to_partner(ref, ref, send, recv)

    to_tp(cbuf.at[tp], cbuf.at[tp], c_send, c_recv)
    swap_cache = to_partner(pc, partner, p_send, p_recv)
    swap_cache.start()
    many(cbuf.at[pl.ds(0, ntp - 1)], c_send, c_recv).wait_recv()

    parts = [cbuf[j] for j in range(ntp)]
    lat = [p[:, 0:128].astype(F32) for p in parts]
    com = [p[:, 128:320].astype(F32) for p in parts]
    lat_mean = sum(jnp.sum(v * v, axis=-1, keepdims=True) for v in lat) / (128.0 * ntp)
    com_mean = sum(jnp.sum(v * v, axis=-1, keepdims=True) for v in com) / (192.0 * ntp)
    lat_scale, com_scale = lax.rsqrt(lat_mean + EPS), lax.rsqrt(com_mean + EPS)
    nope = jnp.zeros((8, 256), F32)
    turned = jnp.zeros((8, 128), F32)
    for j in range(ntp):
        part = (com[j] * com_scale * qgain_v[192 * j : 192 * j + 192][None]).astype(BF)
        nope += dot(part, qu[192 * j : 192 * j + 192])
        turned += dot(part, qr[192 * j : 192 * j + 192])
    turned = rotate(turned.astype(BF).astype(F32), cosine, sine) * SCALE
    nope = nope * SCALE
    for h in range(4):
        qs[pl.ds(h, 8, stride=4), :] = jnp.concatenate(
            [
                nope[:, 64 * h : 64 * h + 64],
                turned[:, 32 * h : 32 * h + 32],
                jnp.zeros((8, 32), F32),
            ],
            axis=1,
        )
    qbuf[0] = qs[0:16].astype(BF)

    @pl.when(core == 0)
    def _():
        pl.semaphore_wait(all_in, 1)

    @pl.when(core == 1)
    def _():
        pl.semaphore_wait(barrier, peers)
        tell(all_in, other_kv, tp)

    for kv_t, unused, slot in targets():
        pltpu.make_async_remote_copy(
            src_ref=qbuf.at[0], dst_ref=qbuf.at[slot], send_sem=q_send, recv_sem=q_recv,
            device_id=(kv_t, tp), device_id_type=MESH,
        ).start()

    for j in range(ntp):
        rows = (lat[j] * lat_scale * lgain_v[:, 128 * j : 128 * j + 128]).astype(BF)
        nb[0:8, 128 * j : 128 * j + 128] = rows
        piece_rows[:, 128 * j : 128 * j + 128] = rows[0:4]
        dec_rows[:, 128 * j : 128 * j + 128] = rows[4:5]
    nb[0:8, 512:640] = rope_row
    piece_rows[:, 512:544] = rope_row[0:4, 0:32]
    dec_rows[:, 512:544] = rope_row[4:5, 0:32]
    swap_rows = to_partner(nb.at[pl.ds(0, 16)], nb.at[pl.ds(16, 16)], n_send, n_recv)
    swap_rows.start()

    head = lax.broadcasted_iota(jnp.int32, (8, 256), 0)
    mine = lax.div(lax.broadcasted_iota(jnp.int32, (8, 256), 1), 64) == head
    alone = jnp.where(mine, jnp.broadcast_to(nope[4:5], (8, 256)), 0.0).astype(BF)
    absorbed = dot(alone, ku[...]).astype(BF)
    dec_turned = qs[16:24, 64:96].astype(BF)
    scores = dot(absorbed, dc[0:512]) + dot(dec_turned, dc[512:544])
    spot = lax.broadcasted_iota(jnp.int32, scores.shape, 1)
    scores = jnp.where(spot < dfill, scores, NEG)
    new_lat = nb[0:8, 0:512].astype(F32)[4:5]
    new_rope = rope_row.astype(F32)[4:5, 0:32]
    new_score = jnp.sum(absorbed.astype(F32) * new_lat, axis=-1, keepdims=True) + jnp.sum(
        dec_turned.astype(F32) * new_rope, axis=-1, keepdims=True
    )
    peak = jnp.maximum(jnp.max(scores, axis=-1, keepdims=True), new_score)
    weights = jnp.exp2(scores - peak)
    new_weight = jnp.exp2(new_score - peak)
    total = jnp.sum(weights, axis=-1, keepdims=True) + new_weight
    mixed = dot_t(weights.astype(BF), dc[0:512]) + new_weight * new_lat
    value = dot_t(mixed.astype(BF), vu[...]) / total
    value = jnp.sum(jnp.where(mine, value, 0.0), axis=0, keepdims=True)
    value = jnp.broadcast_to(value, (8, 256)).astype(BF)
    dbuf[tp] = dot(value, op[...]).astype(BF)
    to_tp(dbuf.at[tp], dbuf.at[tp], d_send, d_recv)

    swap_cache.wait_recv()
    expand(partner, 256)
    swap_rows.wait_recv()
    new_rows = nb[:, 0:512]
    keys = dot_t(ku[...], new_rows).astype(BF)
    vals = dot_t(vu[...], new_rows).astype(BF)
    unit = (
        lax.broadcasted_iota(jnp.int32, (32, 128), 0)
        == lax.broadcasted_iota(jnp.int32, (32, 128), 1)
    ).astype(F32).astype(BF)
    turned_keys = dot_t(unit, nb[:, 512:640]).astype(BF)
    for h in range(4):
        kbuf[h, 0:64, 512:640] = keys[64 * h : 64 * h + 64]
        kbuf[h, 64:96, 512:640] = turned_keys
        vbuf[h, 0:64, 512:640] = vals[64 * h : 64 * h + 64]

    slots = nz * ny
    count = slots * 4
    lane = lax.broadcasted_iota(jnp.int32, (1, 512), 1)
    key_place = jnp.where(lane < 256, kv * 256 + lane, other_kv * 256 + lane - 256)
    old = key_place < fill
    row = lax.broadcasted_iota(jnp.int32, (count, 128), 0)
    slot = lax.div(row, 4)
    src = lax.rem(lax.div(slot, ny) + z, nz) * ny + lax.rem(lax.rem(slot, ny) + y, ny)
    query_token = (src * 2 + core) * 4 + lax.rem(row, 4)
    lane = lax.broadcasted_iota(jnp.int32, (count, 128), 1)
    key_token = jnp.where(lane < 16, kv * 4 + lane, other_kv * 4 + lane - 16)
    fresh = (lax.rem(lane, 16) < 4) & (lane < 32) & (key_token <= query_token)

    many(qbuf.at[pl.ds(1, peers)], q_send, q_recv).wait_recv()
    mid[...] = qbuf[...].reshape(slots * 16, 128).astype(F32)
    for h in range(4):
        queries = mid[pl.ds(h, count, stride=4), :].astype(BF)
        s_old = jnp.where(old, dot(queries, kbuf[h, :, 0:512]), NEG)
        s_new = jnp.where(fresh, dot(queries, kbuf[h, :, 512:640]), NEG)
        peak = jnp.maximum(
            jnp.max(s_old, axis=-1, keepdims=True), jnp.max(s_new, axis=-1, keepdims=True)
        )
        w_old = jnp.exp2(s_old - peak).astype(BF)
        w_new = jnp.exp2(s_new - peak).astype(BF)
        out = dot_t(w_old, vbuf[h, :, 0:512]) + dot_t(w_new, vbuf[h, :, 512:640])
        first = peak.astype(BF).astype(F32)
        second = (peak - first).astype(BF).astype(F32)
        third = peak - first - second
        out = jnp.where(lane == 68, out - out.astype(BF).astype(F32), out)
        out = jnp.where(lane == 65, first, out)
        out = jnp.where(lane == 66, second, out)
        out = jnp.where(lane == 67, third, out)
        mid[pl.ds(h, count, stride=4), :] = out
    rsend[...] = mid[...].astype(BF).reshape(slots, 16, 128)
    rbuf[0] = rsend[0]

    for kv_t, place, slot in targets():
        pltpu.make_async_remote_copy(
            src_ref=rsend.at[place], dst_ref=rbuf.at[slot], send_sem=r_send, recv_sem=r_recv,
            device_id=(kv_t, tp), device_id_type=MESH,
        ).start()

    many(dbuf.at[pl.ds(0, ntp - 1)], d_send, d_recv).wait_recv()
    dec_sum = sum(dbuf[j].astype(F32) for j in range(ntp)).astype(BF)
    dec_out[...] = dec_sum[0:1]
    many(rbuf.at[pl.ds(1, peers)], r_send, r_recv).wait_recv()
    parts = rbuf[...].astype(F32)
    lane = lax.broadcasted_iota(jnp.int32, parts.shape, 2)
    peaks = jnp.sum(
        jnp.where((lane >= 65) & (lane < 68), parts, 0.0), axis=-1, keepdims=True
    )
    factor = jnp.exp2(peaks - jnp.max(peaks, axis=0, keepdims=True))
    merged = jnp.sum(parts * factor, axis=0)
    vs[...] = merged / (merged[:, 64:65] + merged[:, 68:69])
    value = jnp.concatenate([vs[pl.ds(h, 4, stride=4), :][:, 0:64] for h in range(4)], axis=1)
    obuf[tp] = dot(value.astype(BF), op[...]).astype(BF)
    to_tp(obuf.at[tp], obuf.at[tp], o_send, o_recv)
    many(obuf.at[pl.ds(0, ntp - 1)], o_send, o_recv).wait_recv()
    piece_out[...] = sum(obuf[j].astype(F32) for j in range(ntp)).astype(BF)

    many(cbuf.at[pl.ds(0, ntp - 1)], c_send, c_recv).wait_send()
    swap_cache.wait_send()
    swap_rows.wait_send()
    many(qbuf.at[pl.ds(1, peers)], q_send, q_recv).wait_send()
    many(dbuf.at[pl.ds(0, ntp - 1)], d_send, d_recv).wait_send()
    many(rbuf.at[pl.ds(1, peers)], r_send, r_recv).wait_send()
    many(obuf.at[pl.ds(0, ntp - 1)], o_send, o_recv).wait_send()


OUTS = ((4, 2048), (1, 2048), (4, 544), (1, 544))


def store(*refs):
    sems = refs[8]
    copies = [pltpu.make_async_copy(refs[i], refs[4 + i], sems.at[i]) for i in range(4)]
    for copy in copies:
        copy.start()
    for copy in copies:
        copy.wait()


def local(nz, ny, ntp, *args):
    (
        piece_tokens, decode_tokens, prompt_fill, decode_fill, prompt_cache, decode_cache,
        input_gain, query_gain, latent_gain, query_down, latent_down, rope_down,
        query_up, qrope_up, key_up, value_up, out_proj,
    ) = args
    slots = nz * ny
    operands = (
        prompt_fill[None], decode_fill[None], piece_tokens, decode_tokens,
        input_gain[None], query_gain, latent_gain[None],
        query_down.T, latent_down, rope_down.T, query_up, qrope_up,
        key_up.reshape(256, 512), value_up.transpose(0, 2, 1).reshape(256, 512),
        out_proj, prompt_cache.T, decode_cache[0].T,
    )
    copies = [pltpu.VMEM(a.shape, a.dtype) for a in operands]
    dma = pltpu.SemaphoreType.DMA
    any_spec = pl.BlockSpec(memory_space=pltpu.HBM)
    vmem_spec = pl.BlockSpec(memory_space=pltpu.VMEM)
    results = pl.pallas_call(
        functools.partial(kernel, nz, ny, ntp),
        out_shape=tuple(pltpu.VMEM(shape, BF) for shape in OUTS),
        in_specs=[any_spec] * len(operands),
        out_specs=[vmem_spec] * 4,
        scratch_shapes=copies
        + [
            pltpu.VMEM((544, 256), BF),
            pltpu.VMEM((8, 2048), F32),
            pltpu.VMEM((ntp, 8, 384), BF),
            pltpu.VMEM((128, 640), BF),
            pltpu.VMEM((32, 128), F32),
            pltpu.VMEM((4, 128, 640), BF),
            pltpu.VMEM((4, 128, 640), BF),
            pltpu.VMEM((slots, 16, 128), BF),
            pltpu.VMEM((slots, 16, 128), BF),
            pltpu.VMEM((slots, 16, 128), BF),
            pltpu.VMEM((slots * 16, 128), F32),
            pltpu.VMEM((16, 128), F32),
            pltpu.VMEM((ntp, 4, 2048), BF),
            pltpu.VMEM((ntp, 8, 2048), BF),
            pltpu.SemaphoreType.REGULAR,
            pltpu.SemaphoreType.REGULAR,
            pltpu.SemaphoreType.REGULAR,
            dma((len(operands),)),
        ]
        + [dma] * 14,
        compiler_params=pltpu.CompilerParams(collective_id=0, has_side_effects=True),
    )(*operands)
    return pl.pallas_call(
        store,
        out_shape=tuple(jax.ShapeDtypeStruct(shape, BF) for shape in OUTS),
        in_specs=[vmem_spec] * 4,
        out_specs=[any_spec] * 4,
        scratch_shapes=[dma((4,))],
    )(*(pltpu.with_memory_space_constraint(r, pltpu.VMEM) for r in results))


def solution(mesh):
    ntp = mesh.shape["tp"]
    chips = mesh.shape["kv"] // 2
    ny = 1
    while ny * ny < chips:
        ny *= 2
    placed = (
        P("kv", None), P("kv", None), P(), P("kv"), P("kv", None), P("kv", None, None),
        P(), P(), P(), P(None, "tp"), P(None, "tp"), P(), P(None, "tp"), P(None, "tp"),
        P("tp", None, None), P("tp", None, None), P("tp", None),
    )
    return jax.shard_map(
        functools.partial(local, chips // ny, ny, ntp),
        mesh=mesh,
        in_specs=placed,
        out_specs=(P("kv", None),) * 4,
        check_vma=False,
    )
```

```python
import functools

import jax
import jax.numpy as jnp
from jax import lax
from jax.experimental import pallas as pl
from jax.experimental.pallas import tpu as pltpu
from jax.sharding import PartitionSpec as P

MESH = pl.DeviceIdType.MESH
NEG = -1e30
BLOCKS = 2
CHUNK = 32
EPS = 1e-06
LOG2E = 1.4426950408889634
SCALE = (64 + 32) ** (-0.5) * LOG2E
INVERSE = tuple(float(10000.0 ** (-i / 16)) for i in range(16))
BF = jnp.bfloat16
F32 = jnp.float32


def dot(a, b):
    return jnp.dot(a, b, preferred_element_type=F32)


def dot_t(a, b):
    return lax.dot_general(a, b, (((1,), (1,)), ((), ())), preferred_element_type=F32)


def angles(places):
    lane = lax.broadcasted_iota(jnp.int32, (8, 128), 1)
    step = lax.rem(lane, 16)
    inverse = jnp.full((8, 128), INVERSE[0], F32)
    for i in range(1, 16):
        inverse = jnp.where(step == i, INVERSE[i], inverse)
    turn = places.astype(F32) * inverse
    sine = jnp.sin(turn)
    return jnp.cos(turn), jnp.where(lax.rem(lane, 32) < 16, -sine, sine)


def rotate(values, cosine, sine):
    lane = lax.broadcasted_iota(jnp.int32, (8, 128), 1)
    other = jnp.where(
        lax.rem(lane, 32) < 16, pltpu.roll(values, 112, 1), pltpu.roll(values, 16, 1)
    )
    return values * cosine + other * sine


def kernel(
    nz, ny, ntp,
    fill_any, dfill_any, piece_any, dec_any, ingain_any, qgain_any, lgain_any,
    qd_any, ld_any, rd_any, qu_any, qr_any, ku_any, vu_any, op_any, pc_any, dc_any,
    piece_out, dec_out, piece_rows, dec_rows,
    fill_v, dfill_v, piece_v, dec_v, ingain_v, qgain_v, lgain_v,
    qd, ld, rd, qu, qr, ku, vu, op, pc, dc,
    partner, xs, cbuf, nb, kbuf, vbuf, qbuf, rsend, rbuf, psend, pbuf, mid, scores, weights, terms, vs, obuf, dbuf,
    chip_in, line_in, all_in,
    load_sem, c_send, c_recv, p_send, p_recv, n_send, n_recv,
    q_send, q_recv, r_send, r_recv, s_send, s_recv, o_send, o_recv, d_send, d_recv,
):
    kv, tp = lax.axis_index("kv"), lax.axis_index("tp")
    chip, core = lax.div(kv, 2), lax.rem(kv, 2)
    z, y = lax.div(chip, ny), lax.rem(chip, ny)
    peers = nz * ny - 1
    other_kv = chip * 2 + (1 - core)

    pairs = (
        (piece_any, piece_v), (dec_any, dec_v), (ingain_any, ingain_v), (qd_any, qd),
        (ld_any, ld), (pc_any, pc), (ku_any, ku), (vu_any, vu), (rd_any, rd),
        (fill_any, fill_v), (dfill_any, dfill_v), (qgain_any, qgain_v), (lgain_any, lgain_v),
        (qu_any, qu), (qr_any, qr), (dc_any, dc), (op_any, op),
    )
    loads = [pltpu.make_async_copy(a, v, load_sem.at[i]) for i, (a, v) in enumerate(pairs)]
    barrier = pltpu.get_barrier_semaphore()

    z_order = [(p + 1) // 2 if p % 2 else -(p // 2) % nz for p in range(nz)]

    def slot_of(dz, dy):
        return z_order.index(dz % nz) * ny + dy % ny

    z_part = [lax.rem(z + d, nz) * (2 * ny) + core for d in range(nz)]
    y_part = [lax.rem(y + d, ny) * 2 for d in range(ny)]

    def targets():
        def far(step):
            dz, dy = step
            return -(min(dz, nz - dz) + min(dy, ny - dy))

        steps = [(dz, dy) for dz in range(nz) for dy in range(ny)][1:]
        for dz, dy in sorted(steps, key=far):
            yield z_part[dz] + y_part[dy], slot_of(dz, dy), slot_of(-dz, -dy)

    def tell(sem, kv_t, tp_t):
        pl.semaphore_signal(sem, inc=1, device_id=(kv_t, tp_t), device_id_type=MESH)

    beside = sorted(range(1, ntp), key=lambda j: -min(j, ntp - j))

    @pl.when(core == 0)
    def _():
        for j in beside:
            tell(barrier, kv, lax.rem(tp + j, ntp))

    @pl.when(core == 1)
    def _():
        tell(barrier, other_kv, tp)

    for load in loads[:5]:
        load.start()


    @pl.when(core == 0)
    def _():
        pl.semaphore_wait(barrier, ntp)
        tell(chip_in, other_kv, tp)
        for j in beside:
            tell(line_in, kv, lax.rem(tp + j, ntp))

    @pl.when(core == 1)
    def _():
        pl.semaphore_wait(chip_in, 1)
        for kv_t, unused, unused_too in targets():
            tell(barrier, kv_t, tp)

    for load in loads[5:]:
        load.start()

    kbuf[...] = jnp.zeros(kbuf.shape, BF)
    nb[0:16] = jnp.zeros((16, 640), BF)
    nb[32:128] = jnp.zeros((96, 640), BF)
    xs[...] = jnp.zeros(xs.shape, F32)
    for load in loads[:5]:
        load.wait()
    xs[0:4] = piece_v[...].astype(F32)
    xs[4:5] = dec_v[...].astype(F32)
    x = xs[...]
    mean = jnp.mean(x * x, axis=-1, keepdims=True)
    normed = (x * lax.rsqrt(mean + EPS) * ingain_v[...]).astype(BF)
    cbuf[tp, :, 0:128] = dot(normed, ld[...]).astype(BF)
    cbuf[tp, :, 128:320] = dot_t(normed, qd[...]).astype(BF)

    @pl.when(core == 0)
    def _():
        pl.semaphore_wait(line_in, ntp - 1)
        tell(chip_in, other_kv, tp)

    @pl.when(core == 1)
    def _():
        pl.semaphore_wait(chip_in, 1)

    def to_tp(src, dst, send, recv):
        for j in beside:
            pltpu.make_async_remote_copy(
                src_ref=src, dst_ref=dst, send_sem=send, recv_sem=recv,
                device_id=(kv, lax.rem(tp + j, ntp)), device_id_type=MESH,
            ).start()

    def to_partner(src, dst, send, recv):
        return pltpu.make_async_remote_copy(
            src_ref=src, dst_ref=dst, send_sem=send, recv_sem=recv,
            device_id=(other_kv, tp), device_id_type=MESH,
        )

    def many(ref, send, recv):
        return to_partner(ref, ref, send, recv)

    to_tp(cbuf.at[tp], cbuf.at[tp], c_send, c_recv)
    loads[5].wait()
    swap_cache = to_partner(pc, partner, p_send, p_recv)
    swap_cache.start()

    for load in loads[6:9]:
        load.wait()

    def keep_keys(keys, turned_keys, at):
        width = keys.shape[1]
        for h in range(4):
            own, rope = h % 2 * 64, 128 + 32 * h
            kbuf[h, own : own + 64, at : at + width] = keys[64 * h : 64 * h + 64]
            kbuf[h, rope : rope + 32, at : at + width] = turned_keys

    def keep_values(vals, at):
        half = lax.div(lax.broadcasted_iota(jnp.int32, (vals.shape[0], 128), 1), 64)
        for h in range(4):
            pair = vals[:, h // 2 * 128 : h // 2 * 128 + 128]
            vbuf[h, at : at + vals.shape[0]] = jnp.where(half == h % 2, pair, 0.0).astype(BF)

    def expand(rows, at):
        latent = rows[0:512]
        keys = dot(ku[...], latent).astype(BF)
        turned_keys = rows[512:544]
        keep_keys(keys, turned_keys, at)
        keep_values(dot(vu[...], latent).T, at)

    expand(pc, 0)
    rope_raw = dot_t(normed, rd[...]).astype(BF).astype(F32)
    for load in loads[9:]:
        load.wait()
    fill, dfill = fill_v[...], dfill_v[...]
    token_row = lax.broadcasted_iota(jnp.int32, (8, 128), 0)
    places = jnp.where(token_row < 4, fill + kv * 4 + token_row, dfill)
    cosine, sine = angles(places)
    rope_row = rotate(
        jnp.concatenate([rope_raw, jnp.zeros((8, 96), F32)], axis=1), cosine, sine
    ).astype(BF)

    many(cbuf.at[pl.ds(0, ntp - 1)], c_send, c_recv).wait_recv()

    parts = [cbuf[j] for j in range(ntp)]
    lat = [p[:, 0:128].astype(F32) for p in parts]
    com = [p[:, 128:320].astype(F32) for p in parts]
    lat_mean = sum(jnp.sum(v * v, axis=-1, keepdims=True) for v in lat) / (128.0 * ntp)
    com_mean = sum(jnp.sum(v * v, axis=-1, keepdims=True) for v in com) / (192.0 * ntp)
    lat_scale, com_scale = lax.rsqrt(lat_mean + EPS), lax.rsqrt(com_mean + EPS)
    nope = jnp.zeros((8, 256), F32)
    turned = jnp.zeros((8, 128), F32)
    for j in range(ntp):
        part = (com[j] * com_scale * qgain_v[192 * j : 192 * j + 192][None]).astype(BF)
        nope += dot(part, qu[192 * j : 192 * j + 192])
        turned += dot(part, qr[192 * j : 192 * j + 192])
    turned = rotate(turned.astype(BF).astype(F32), cosine, sine) * SCALE
    nope = nope * SCALE
    qbuf[0, 0] = nope[0:4, 0:128].astype(BF)
    qbuf[0, 1] = nope[0:4, 128:256].astype(BF)
    qbuf[0, 2] = turned[0:4].astype(BF)

    @pl.when(core == 0)
    def _():
        pl.semaphore_wait(all_in, 1)

    @pl.when(core == 1)
    def _():
        pl.semaphore_wait(barrier, peers)
        tell(all_in, other_kv, tp)

    for kv_t, unused, slot in targets():
        pltpu.make_async_remote_copy(
            src_ref=qbuf.at[0], dst_ref=qbuf.at[slot],
            send_sem=q_send, recv_sem=q_recv.at[slot // (nz * ny // BLOCKS)],
            device_id=(kv_t, tp), device_id_type=MESH,
        ).start()

    for j in range(ntp):
        rows = (lat[j] * lat_scale * lgain_v[:, 128 * j : 128 * j + 128]).astype(BF)
        nb[0:8, 128 * j : 128 * j + 128] = rows
        piece_rows[:, 128 * j : 128 * j + 128] = rows[0:4]
        dec_rows[:, 128 * j : 128 * j + 128] = rows[4:5]
    nb[0:8, 512:640] = rope_row
    piece_rows[:, 512:544] = rope_row[0:4, 0:32]
    dec_rows[:, 512:544] = rope_row[4:5, 0:32]
    swap_rows = to_partner(nb.at[pl.ds(0, 16)], nb.at[pl.ds(16, 16)], n_send, n_recv)
    swap_rows.start()

    head = lax.broadcasted_iota(jnp.int32, (8, 256), 0)
    mine = lax.div(lax.broadcasted_iota(jnp.int32, (8, 256), 1), 64) == head
    alone = jnp.where(mine, jnp.broadcast_to(nope[4:5], (8, 256)), 0.0).astype(BF)
    absorbed = dot(alone, ku[...]).astype(BF)
    dec_turned = jnp.where(
        lax.div(lax.broadcasted_iota(jnp.int32, (8, 128), 1), 32) == token_row, turned[4:5], 0.0
    )
    dec_turned = dec_turned + pltpu.roll(dec_turned, 64, 1)
    dec_turned = (dec_turned + pltpu.roll(dec_turned, 96, 1))[:, 0:32].astype(BF)
    dec_scores = dot(absorbed, dc[0:512]) + dot(dec_turned, dc[512:544])
    spot = lax.broadcasted_iota(jnp.int32, dec_scores.shape, 1)
    dec_scores = jnp.where(spot < dfill, dec_scores, NEG)
    new_lat = nb[0:8, 0:512].astype(F32)[4:5]
    new_rope = rope_row.astype(F32)[4:5, 0:32]
    new_score = jnp.sum(absorbed.astype(F32) * new_lat, axis=-1, keepdims=True) + jnp.sum(
        dec_turned.astype(F32) * new_rope, axis=-1, keepdims=True
    )
    peak = jnp.maximum(jnp.max(dec_scores, axis=-1, keepdims=True), new_score)
    dec_weights = jnp.exp2(dec_scores - peak)
    new_weight = jnp.exp2(new_score - peak)
    total = jnp.sum(dec_weights, axis=-1, keepdims=True) + new_weight
    mixed = dot_t(dec_weights.astype(BF), dc[0:512]) + new_weight * new_lat
    value = dot_t(mixed.astype(BF), vu[...]) / total
    value = jnp.sum(jnp.where(mine, value, 0.0), axis=0, keepdims=True)
    value = jnp.broadcast_to(value, (8, 256)).astype(BF)
    dbuf[tp] = dot(value, op[...]).astype(BF)
    to_tp(dbuf.at[tp], dbuf.at[tp], d_send, d_recv)

    swap_cache.wait_recv()
    expand(partner, 256)
    swap_rows.wait_recv()
    new_rows = nb[:, 0:512]
    keys = dot_t(ku[...], new_rows).astype(BF)
    keep_values(dot_t(new_rows, vu[...]), 512)
    unit = (
        lax.broadcasted_iota(jnp.int32, (32, 128), 0)
        == lax.broadcasted_iota(jnp.int32, (32, 128), 1)
    ).astype(F32).astype(BF)
    turned_keys = dot_t(unit, nb[:, 512:640]).astype(BF)
    keep_keys(keys, turned_keys, 512)

    lane = lax.broadcasted_iota(jnp.int32, (1, 512), 1)
    key_place = jnp.where(lane < 256, kv * 256 + lane, other_kv * 256 + lane - 256)
    old = key_place < fill
    slots = nz * ny // BLOCKS
    count = slots * 4
    row = lax.broadcasted_iota(jnp.int32, (count, 128), 0)
    lane = lax.broadcasted_iota(jnp.int32, (count, 128), 1)
    key_token = jnp.where(lane < 16, kv * 4 + lane, other_kv * 4 + lane - 16)
    within = jnp.where(lane < 32, lax.rem(lane, 16) - 4 * lax.rem(row, 4), -1)
    is_new = (lax.rem(lane, 16) < 4) & (lane < 32)

    def attend(block):
        base = block * slots
        slot = lax.div(row, 4) + base
        turn = lax.div(slot, ny)
        dz = jnp.where(
            lax.rem(turn, 2) == 1, lax.div(turn + 1, 2), lax.rem(nz - lax.div(turn, 2), nz)
        )
        src = lax.rem(dz + z, nz) * ny + lax.rem(lax.rem(slot, ny) + y, ny)
        query_token = (src * 2 + core) * 4 + lax.rem(row, 4)
        fresh = is_new & (key_token <= query_token)
        got = [
            qbuf[base : base + slots, g].astype(F32).reshape(count, 128).astype(BF) for g in range(3)
        ]
        for h in range(4):
            queries = jnp.concatenate([got[h // 2], got[2]], axis=1)
            scores[h] = dot(queries, kbuf[h])
        for at in range(0, count, CHUNK):
            part = slice(at, at + CHUNK)
            scalars = jnp.zeros((CHUNK, 128), F32)
            for h in range(4):
                s_old = jnp.where(old, scores[h, part, 0:512], NEG)
                s_new = jnp.where(fresh[part], scores[h, part, 512:640], NEG)
                peak = jnp.ceil(
                    jnp.maximum(
                        jnp.max(s_old, axis=-1, keepdims=True),
                        jnp.max(s_new, axis=-1, keepdims=True),
                    )
                )
                w_old = jnp.exp2(s_old - peak)
                w_new = jnp.exp2(s_new - peak)
                total = jnp.sum(w_old, axis=-1, keepdims=True) + jnp.sum(
                    w_new, axis=-1, keepdims=True
                )
                weights[h, part, 0:512] = w_old.astype(BF)
                weights[h, part, 512:640] = w_new.astype(BF)
                scalar = jnp.where(lane[part] < 16, peak, total)
                scalars = jnp.where(within[part] == h, scalar, scalars)
            terms[part] = scalars
        for pair in range(2):
            h = 2 * pair
            mid[pl.ds(pair, count, stride=2), :] = dot(weights[h], vbuf[h]) + dot(
                weights[h + 1], vbuf[h + 1]
            )
        rsend[base : base + slots] = mid[...].astype(BF).reshape(slots, 8, 128)
        gather = lax.div(lax.broadcasted_iota(jnp.int32, (slots, count), 1), 4)
        gather = gather == lax.broadcasted_iota(jnp.int32, (slots, count), 0)
        rows = jnp.dot(
            gather.astype(F32), terms[...],
            preferred_element_type=F32, precision=lax.Precision.HIGHEST,
        )
        psend[base : base + slots] = rows[:, None, :]

    for block in reversed(range(BLOCKS)):
        base = block * slots
        first = max(base, 1)
        many(qbuf.at[pl.ds(first, base + slots - first)], q_send, q_recv.at[block]).wait_recv()
        attend(block)
        if block == 0:
            rbuf[0] = rsend[0]
            pbuf[0] = psend[0]
        for kv_t, place, slot in targets():
            if place // slots == block:
                pltpu.make_async_remote_copy(
                    src_ref=rsend.at[place], dst_ref=rbuf.at[slot],
                    send_sem=r_send, recv_sem=r_recv,
                    device_id=(kv_t, tp), device_id_type=MESH,
                ).start()
                pltpu.make_async_remote_copy(
                    src_ref=psend.at[place], dst_ref=pbuf.at[slot],
                    send_sem=s_send, recv_sem=s_recv,
                    device_id=(kv_t, tp), device_id_type=MESH,
                ).start()

    many(dbuf.at[pl.ds(0, ntp - 1)], d_send, d_recv).wait_recv()
    dec_sum = sum(dbuf[j].astype(F32) for j in range(ntp)).astype(BF)
    dec_out[...] = dec_sum[0:1]
    many(rbuf.at[pl.ds(1, peers)], r_send, r_recv).wait_recv()
    many(pbuf.at[pl.ds(1, peers)], s_send, s_recv).wait_recv()
    scalars = pbuf[...]
    factor = jnp.exp2(scalars - jnp.max(scalars, axis=0, keepdims=True))
    totals = pltpu.roll(scalars, 112, 2)
    every = scalars.shape[0]
    lane = lax.broadcasted_iota(jnp.int32, (1, 1, 128), 2)
    factor = jnp.where(lane < 16, factor, 0.0)
    total = jnp.sum(factor * totals, axis=0)
    mine = lax.div(lax.broadcasted_iota(jnp.int32, (1, 8, 128), 2), 2)
    mine = mine == lax.broadcasted_iota(jnp.int32, (1, 8, 128), 1)
    spread = lax.rem(lax.broadcasted_iota(jnp.int32, (128, 128), 0), 2)
    spread = spread == lax.div(lax.broadcasted_iota(jnp.int32, (128, 128), 1), 64)
    spread = spread.astype(F32)
    factor = jnp.where(mine, factor, 0.0).reshape(every * 8, 128).astype(BF)
    factor = dot(factor, spread.astype(BF)).reshape(every, 8, 128)
    total = jnp.dot(
        jnp.where(mine[0], total, 0.0), spread,
        preferred_element_type=F32, precision=lax.Precision.HIGHEST,
    )
    merged = jnp.sum(rbuf[...].astype(F32) * factor, axis=0)
    vs[...] = merged / total
    value = jnp.concatenate([vs[pl.ds(p, 4, stride=2), :] for p in range(2)], axis=1)
    obuf[tp] = dot(value.astype(BF), op[...]).astype(BF)
    to_tp(obuf.at[tp], obuf.at[tp], o_send, o_recv)
    many(obuf.at[pl.ds(0, ntp - 1)], o_send, o_recv).wait_recv()
    piece_out[...] = sum(obuf[j].astype(F32) for j in range(ntp)).astype(BF)

    many(cbuf.at[pl.ds(0, ntp - 1)], c_send, c_recv).wait_send()
    swap_cache.wait_send()
    swap_rows.wait_send()
    many(qbuf.at[pl.ds(1, peers)], q_send, q_recv.at[0]).wait_send()
    many(dbuf.at[pl.ds(0, ntp - 1)], d_send, d_recv).wait_send()
    many(rbuf.at[pl.ds(1, peers)], r_send, r_recv).wait_send()
    many(pbuf.at[pl.ds(1, peers)], s_send, s_recv).wait_send()
    many(obuf.at[pl.ds(0, ntp - 1)], o_send, o_recv).wait_send()


OUTS = ((4, 2048), (1, 2048), (4, 544), (1, 544))


def store(*refs):
    sems = refs[8]
    copies = [pltpu.make_async_copy(refs[i], refs[4 + i], sems.at[i]) for i in range(4)]
    for copy in copies:
        copy.start()
    for copy in copies:
        copy.wait()


def local(nz, ny, ntp, *args):
    (
        piece_tokens, decode_tokens, prompt_fill, decode_fill, prompt_cache, decode_cache,
        input_gain, query_gain, latent_gain, query_down, latent_down, rope_down,
        query_up, qrope_up, key_up, value_up, out_proj,
    ) = args
    slots = nz * ny
    operands = (
        prompt_fill[None], decode_fill[None], piece_tokens, decode_tokens,
        input_gain[None], query_gain, latent_gain[None],
        query_down.T, latent_down, rope_down.T, query_up, qrope_up,
        key_up.reshape(256, 512), value_up.transpose(0, 2, 1).reshape(256, 512),
        out_proj, prompt_cache.T, decode_cache[0].T,
    )
    copies = [pltpu.VMEM(a.shape, a.dtype) for a in operands]
    dma = pltpu.SemaphoreType.DMA
    any_spec = pl.BlockSpec(memory_space=pltpu.HBM)
    vmem_spec = pl.BlockSpec(memory_space=pltpu.VMEM)
    results = pl.pallas_call(
        functools.partial(kernel, nz, ny, ntp),
        out_shape=tuple(pltpu.VMEM(shape, BF) for shape in OUTS),
        in_specs=[any_spec] * len(operands),
        out_specs=[vmem_spec] * 4,
        scratch_shapes=copies
        + [
            pltpu.VMEM((544, 256), BF),
            pltpu.VMEM((8, 2048), F32),
            pltpu.VMEM((ntp, 8, 384), BF),
            pltpu.VMEM((128, 640), BF),
            pltpu.VMEM((4, 256, 640), BF),
            pltpu.VMEM((4, 640, 128), BF),
            pltpu.VMEM((slots, 3, 4, 128), BF),
            pltpu.VMEM((slots, 8, 128), BF),
            pltpu.VMEM((slots, 8, 128), BF),
            pltpu.VMEM((slots, 1, 128), F32),
            pltpu.VMEM((slots, 1, 128), F32),
            pltpu.VMEM((slots // BLOCKS * 8, 128), F32),
            pltpu.VMEM((4, slots // BLOCKS * 4, 640), F32),
            pltpu.VMEM((4, slots // BLOCKS * 4, 640), BF),
            pltpu.VMEM((slots // BLOCKS * 4, 128), F32),
            pltpu.VMEM((8, 128), F32),
            pltpu.VMEM((ntp, 4, 2048), BF),
            pltpu.VMEM((ntp, 8, 2048), BF),
            pltpu.SemaphoreType.REGULAR,
            pltpu.SemaphoreType.REGULAR,
            pltpu.SemaphoreType.REGULAR,
            dma((len(operands),)),
        ]
        + [dma] * 7
        + [dma((BLOCKS,))]
        + [dma] * 8,
        compiler_params=pltpu.CompilerParams(collective_id=0, has_side_effects=True),
    )(*operands)
    return pl.pallas_call(
        store,
        out_shape=tuple(jax.ShapeDtypeStruct(shape, BF) for shape in OUTS),
        in_specs=[vmem_spec] * 4,
        out_specs=[any_spec] * 4,
        scratch_shapes=[dma((4,))],
    )(*(pltpu.with_memory_space_constraint(r, pltpu.VMEM) for r in results))


def solution(mesh):
    ntp = mesh.shape["tp"]
    chips = mesh.shape["kv"] // 2
    ny = 1
    while ny * ny < chips:
        ny *= 2
    placed = (
        P("kv", None), P("kv", None), P(), P("kv"), P("kv", None), P("kv", None, None),
        P(), P(), P(), P(None, "tp"), P(None, "tp"), P(), P(None, "tp"), P(None, "tp"),
        P("tp", None, None), P("tp", None, None), P("tp", None),
    )
    return jax.shard_map(
        functools.partial(local, chips // ny, ny, ntp),
        mesh=mesh,
        in_specs=placed,
        out_specs=(P("kv", None),) * 4,
        check_vma=False,
    )
```
